1024 devices in a mesh: ep: 64 (over z, y), tp: 16 (over x, core).
Axes of the slice: x: 8, y: 8, z: 8, core: 2. Of those that a mesh axis runs over, the one named last changes fastest.
Arguments:
- tokens: bfloat16 [8192, 2048], P('ep'), may hold values from -6 to 6
- norm_gain: float32 [2048], replicated, may hold values from 0.1 to 1.9
- expert_ids: int32 [8192, 6], P('ep'), may hold values from 0 to 511, all different within a row; in each aligned block of 128 rows (0 to 127, 128 to 255, ...) at most 2 rows name the same one
- route_weights: float32 [8192, 6], P('ep'), may hold values from 0.1 to 1
- expert_gate: bfloat16 [1024, 2048, 256], P(('ep', 'tp')), may hold values from -0.125 to 0.125
- expert_up: bfloat16 [1024, 2048, 256], P(('ep', 'tp')), may hold values from -0.125 to 0.125
- expert_down: bfloat16 [1024, 256, 2048], P(('ep', 'tp')), may hold values from -0.25 to 0.25
- shared_gate: bfloat16 [2048, 512], P(None, 'tp'), may hold values from -0.125 to 0.125
- shared_up: bfloat16 [2048, 512], P(None, 'tp'), may hold values from -0.125 to 0.125
- shared_down: bfloat16 [512, 2048], P(None, 'tp'), may hold values from -0.25 to 0.25
Outputs:
- mixed: bfloat16 [8192, 2048], P('ep', 'tp')
The draws below stay inside these ranges and needn't reach their ends.
Inputs may be any that keep to these rules, and one draw needn't show every extreme that they name: `expert_ids`: each row names 6 different experts. In each aligned block of 128 rows (the rows of one index of ep) no expert is named by more than 2 rows, a bound that some block reaches.
All inputs are finite; a program needn't handle non-finite values.
Results may differ from the reference program's by a relative error of at most 0.0073.
Values may be sent and summed in bfloat16 or wider, within the bound.
No kernel may reach another device: no remote copies, remote signals or barrier semaphores. Data moves between devices by JAX's collectives and lax.ppermute only.
A program may use at most 32 MiB of HBM per device.

```python
import math
import jax
import jax.numpy as jnp
import numpy as np
from jax import lax

D = 2048
EXPERT_FF = 512
SHARED_FF = 512
TOP_K = 6
TOK_DEV = 128
EXP_HALF = 256
EXPERTS = 512
CAP = 2
TOKENS = 8192
N_EP = 64


def level_of(stream_key, extent, split, low, high):
    def one(dim, shards_of):
        heights = jax.random.uniform(jax.random.fold_in(jax.random.fold_in(stream_key, 6), dim), (shards_of,), jnp.float32, low / len(split), high / len(split))
        return jnp.repeat(jnp.exp(heights), extent[dim] // shards_of).reshape((-1,) + (1,) * (len(extent) - dim - 1))

    loudness = one(*split[0])
    for cut in split[1:]:
        loudness = loudness * one(*cut)
    return loudness


def deal_out(rng, own, number, rows, amount, top, bound, slope):
    ranking = jax.random.permutation(rng, amount)
    crowded, usual = portions_of(amount, rows * top, bound, slope, True), portions_of(amount, rows * top, bound, slope, False)
    places = jnp.arange(amount)

    def named(tallies, turn):
        used = int((tallies > 0).sum())
        fixed = max(1, used // 4)
        passed = fixed + (places - fixed + turn * (used - fixed)) % max(1, amount - fixed)
        return jnp.zeros((amount,), jnp.int32).at[ranking[jnp.where(places < fixed, places, passed)]].set(jnp.asarray(tallies, jnp.int32))

    tallies = jnp.where(number % 4 == 0, named(crowded, number // 4), named(usual, number - number // 4 - 1))
    mixed = jax.random.permutation(jax.random.fold_in(own, 3), amount)
    donor, taker = mixed[0:amount // 2 * 2:2], mixed[1:amount // 2 * 2:2]
    room = jnp.minimum(tallies[donor] - 1, bound - tallies[taker]) // 2
    room = jnp.where((donor == ranking[0]) | (taker == ranking[0]) | (tallies[taker] == 0), 0, jnp.maximum(room, 0))
    passed = jax.random.randint(jax.random.fold_in(own, 4), (amount // 2,), 0, 1 << 20) % (room + 1)
    tallies = tallies.at[donor].add(-passed).at[taker].add(passed)
    labels = jnp.searchsorted(jnp.cumsum(tallies), jnp.arange(rows * top), side="right").astype(jnp.int32)
    listing = labels.reshape(top, rows).T
    listing = listing[jax.random.permutation(jax.random.fold_in(own, 1), rows)]
    turn = jax.random.randint(jax.random.fold_in(own, 2), (rows, 1), 0, top)
    return jnp.take_along_axis(listing, (jnp.arange(top)[None, :] + turn) % top, axis=1)


def portions_of(count, total, reach, slope, full):
    loads = [(1 << 20) // math.isqrt(grade ** slope) + 1 for grade in range(1, count + 1)]
    largest = reach if full else min(reach, max(-(-total // count), total * loads[0] // sum(loads)))
    least = 1 if total - largest >= count - 1 else 0
    given, spare = [largest] + [least] * (count - 1), total - largest - least * (count - 1)
    while spare > 0:
        movable = [i for i in range(1, count) if given[i] < largest] or [i for i in range(1, count) if given[i] < reach]
        mass, budget = sum([loads[i] for i in movable]), spare
        for i in movable:
            addition = min(reach - given[i], max(1, budget * loads[i] // mass), spare)
            given[i] = given[i] + addition
            spare = spare - addition
    return np.array(given)


def bell_draw(stream_key, extent, spread, most, cuts=(), held_as=jnp.bfloat16):
    array = spread * jax.random.normal(stream_key, extent, jnp.float32)
    if cuts:
        array = array * level_of(stream_key, extent, cuts, -0.22, 0.18)
    return jnp.clip(array, -most, most).astype(held_as)


def setup_inputs(seed: int = 0) -> dict:
    keys = jax.random.split(jax.random.key(seed), 11)
    tokens = bell_draw(keys[0], (TOKENS, D), 1.0, 6.0, ((0, 64),))
    norm_gain = jnp.clip(1.0 + 0.18 * jax.random.normal(keys[1], (D,), jnp.float32), 0.1, 1.9)
    expert_ids_keys = jax.random.split(jax.random.fold_in(keys[2], 1), TOKENS // TOK_DEV)
    expert_ids_turns = jax.random.permutation(jax.random.fold_in(keys[2], 3), TOKENS // TOK_DEV)
    expert_ids = jax.vmap(lambda own, number: deal_out(jax.random.fold_in(keys[2], 2), own, number, TOK_DEV, EXPERTS, TOP_K, CAP, 2))(expert_ids_keys, expert_ids_turns).reshape((TOKENS, TOP_K))
    route_weights = jnp.clip(jnp.exp(math.log(1.0) - 2.3025851 * jax.random.uniform(keys[3], (TOKENS, TOP_K), jnp.float32) ** level_of(keys[3], (TOKENS, TOP_K), ((0, 64),), -0.2, 0.2)), 0.1, 1.0)
    expert_gate = bell_draw(keys[4], (2 * EXPERTS, D, EXP_HALF), D ** -0.5, 0.125, ((0, 1024),))
    expert_up = bell_draw(keys[5], (2 * EXPERTS, D, EXP_HALF), D ** -0.5, 0.125, ((0, 1024),))
    expert_down = bell_draw(keys[6], (2 * EXPERTS, EXP_HALF, D), EXPERT_FF ** -0.5, 0.25, ((0, 1024),))
    shared_gate = bell_draw(keys[7], (D, SHARED_FF), D ** -0.5, 0.125, ((1, 16),))
    shared_up = bell_draw(keys[8], (D, SHARED_FF), D ** -0.5, 0.125, ((1, 16),))
    shared_down = bell_draw(keys[9], (SHARED_FF, D), SHARED_FF ** -0.5, 0.25, ((1, 16),))
    return {"tokens": tokens, "norm_gain": norm_gain, "expert_ids": expert_ids, "route_weights": route_weights, "expert_gate": expert_gate, "expert_up": expert_up, "expert_down": expert_down, "shared_gate": shared_gate, "shared_up": shared_up, "shared_down": shared_down}


NORM_EPSILON = 1e-06

def rms_normed(tokens, norm_gain):
    as_float = tokens.astype(jnp.float32)
    inverse_rms = lax.rsqrt(lax.optimization_barrier(jnp.mean(as_float * as_float, axis=-1, keepdims=True)) + NORM_EPSILON)
    return (as_float * inverse_rms * norm_gain).astype(jnp.bfloat16)

def slot_numbers(expert_ids, block_rows, expert_count):
    expert_iota = jnp.arange(expert_count, dtype=jnp.int32)
    counts = lax.optimization_barrier(jnp.sum((expert_ids[:, :, None] == expert_iota[None, None, :]).astype(jnp.int32), axis=1))
    blocked = counts.reshape(-1, block_rows, expert_count)
    prefix = (jnp.cumsum(blocked, axis=1) - blocked).reshape(counts.shape)
    return jnp.take_along_axis(prefix, expert_ids, axis=1).astype(jnp.int32)

def half_output(gathered, gate_half, up_half, down_half):
    hidden = (jax.nn.silu(jnp.dot(gathered, gate_half, preferred_element_type=jnp.float32)) * jnp.dot(gathered, up_half, preferred_element_type=jnp.float32)).astype(jnp.bfloat16)
    rounded = jnp.dot(hidden, down_half, preferred_element_type=jnp.float32).astype(jnp.bfloat16)
    return lax.optimization_barrier(rounded).astype(jnp.float32)

def reference(tokens, norm_gain, expert_ids, route_weights, expert_gate, expert_up, expert_down, shared_gate, shared_up, shared_down):
    normed = rms_normed(tokens, norm_gain)
    token_count, model_width = tokens.shape
    block_rows = token_count // N_EP
    slot_index = slot_numbers(expert_ids, block_rows, EXPERTS)
    token_iota = jnp.arange(token_count, dtype=jnp.int32)
    source_block = jnp.broadcast_to((token_iota // block_rows)[:, None], expert_ids.shape).astype(jnp.int32)
    token_rows = jnp.broadcast_to(token_iota[:, None], expert_ids.shape).astype(jnp.int32)
    token_table = jnp.full((EXPERTS, N_EP, CAP), token_count, jnp.int32)
    token_table = token_table.at[expert_ids, source_block, slot_index].set(token_rows)
    weight_table = jnp.zeros((EXPERTS, N_EP, CAP), jnp.float32)
    weight_table = weight_table.at[expert_ids, source_block, slot_index].set(route_weights)
    padded = jnp.concatenate([normed, jnp.zeros((1, model_width), jnp.bfloat16)], axis=0)
    gate_pairs = expert_gate.reshape(EXPERTS, 2, model_width, EXP_HALF)
    up_pairs = expert_up.reshape(EXPERTS, 2, model_width, EXP_HALF)
    down_pairs = expert_down.reshape(EXPERTS, 2, EXP_HALF, model_width)

    def expert_step(running, inputs):
        gate_two, up_two, down_two, table_rows, table_weights = inputs
        flat_tokens = table_rows.reshape(-1)
        gathered = padded[flat_tokens]
        first = half_output(gathered, gate_two[0], up_two[0], down_two[0])
        second = half_output(gathered, gate_two[1], up_two[1], down_two[1])
        output = (first + second).astype(jnp.bfloat16)
        running = running.at[flat_tokens].add(output.astype(jnp.float32) * table_weights.reshape(-1)[:, None])
        return (running, None)
    start = jnp.zeros((token_count + 1, model_width), jnp.float32)
    routed, _ = lax.scan(expert_step, start, (gate_pairs, up_pairs, down_pairs, token_table, weight_table))
    shared_act = (jax.nn.silu(jnp.dot(normed, shared_gate, preferred_element_type=jnp.float32)) * jnp.dot(normed, shared_up, preferred_element_type=jnp.float32)).astype(jnp.bfloat16)
    shared_out = jnp.dot(shared_act, shared_down, preferred_element_type=jnp.float32)
    return (routed[:token_count] + shared_out).astype(jnp.bfloat16)
```

```python
import jax
import jax.numpy as jnp
from jax import lax
from jax.sharding import Mesh
from jax.sharding import PartitionSpec as P

TP = ("x", "core")
EP = ("z", "y")
ALL = ("z", "y", "x", "core")

NORM_EPSILON = 1e-06


def dot(a, b, dims=((1,), (0,))):
    return lax.dot_general(a, b, (dims, ((), ())), preferred_element_type=jnp.float32)


def local(
    tokens,
    norm_gain,
    expert_ids,
    route_weights,
    expert_gate,
    expert_up,
    expert_down,
    shared_gate,
    shared_up,
    shared_down,
):
    groups = lax.axis_size(EP)
    columns = lax.axis_size("x")
    cores = lax.axis_size("core")
    column = lax.axis_index("x")
    core = lax.axis_index("core")
    rows, width = tokens.shape
    top_count = expert_ids.shape[1]
    cap = 2
    slots = groups * cap
    block = width // (columns * cores)

    as_float = tokens.astype(jnp.float32)
    inverse_rms = lax.rsqrt(jnp.mean(as_float * as_float, axis=-1, keepdims=True) + NORM_EPSILON)
    normed = (as_float * inverse_rms * norm_gain).astype(jnp.bfloat16)

    token_iota = jnp.arange(rows, dtype=jnp.int32)
    strict_lower = (token_iota[:, None] > token_iota[None, :]).astype(jnp.bfloat16)

    slot_iota = jnp.arange(slots, dtype=jnp.int32)
    slot_expert = (slot_iota // cap) * columns + column
    named = jnp.zeros((rows, slots), jnp.bool_)
    for k in range(top_count):
        named = named | (expert_ids[:, k : k + 1] == slot_expert[None, :])
    earlier = dot(strict_lower, named.astype(jnp.bfloat16))
    chosen = named & (earlier == (slot_iota % cap).astype(jnp.float32)[None, :])
    buffer = dot(chosen.astype(jnp.bfloat16), normed, ((0,), (0,))).astype(jnp.bfloat16)
    buffer = buffer.reshape(groups, cap, width)
    received = lax.all_to_all(buffer, EP, split_axis=0, concat_axis=0, tiled=True)

    shared_act = (
        jax.nn.silu(dot(shared_gate, normed, ((0,), (1,)))) * dot(shared_up, normed, ((0,), (1,)))
    ).astype(jnp.bfloat16)
    other_act = lax.ppermute(shared_act, "core", [(0, 1), (1, 0)])
    pair_act = jnp.where(
        core == 0,
        jnp.concatenate([shared_act, other_act], 0),
        jnp.concatenate([other_act, shared_act], 0),
    )

    all_iota = jnp.arange(columns * groups, dtype=jnp.int32)
    all_expert = (all_iota % groups) * columns + all_iota // groups
    weight = jnp.zeros((rows, columns * groups), jnp.float32)
    taken = jnp.zeros((rows, columns * groups), jnp.bool_)
    for k in range(top_count):
        hit = expert_ids[:, k : k + 1] == all_expert[None, :]
        taken = taken | hit
        weight = jnp.where(hit, route_weights[:, k : k + 1], weight)
    ahead = dot(strict_lower, taken.astype(jnp.bfloat16))

    flat_rows = received.reshape(slots, width)
    hidden = (
        jax.nn.silu(dot(flat_rows, expert_gate[0])) * dot(flat_rows, expert_up[0])
    ).astype(jnp.bfloat16)
    down = expert_down[0].reshape(-1, columns, cores, block)
    down_kept = lax.dynamic_index_in_dim(down, core, 2, keepdims=False).reshape(-1, width // cores)
    down_sent = lax.dynamic_index_in_dim(down, 1 - core, 2, keepdims=False).reshape(-1, width // cores)
    sent = dot(hidden, down_sent).astype(jnp.bfloat16)
    partner = lax.ppermute(sent, "core", [(0, 1), (1, 0)])
    kept = dot(hidden, down_kept).astype(jnp.bfloat16)
    expert_out = (kept.astype(jnp.float32) + partner.astype(jnp.float32)).astype(jnp.bfloat16)
    returned = lax.all_to_all(
        expert_out.reshape(groups, cap, columns * block), EP, split_axis=0, concat_axis=0, tiled=True
    )
    by_column = jnp.moveaxis(returned.reshape(slots, columns, block), 1, 0)
    payload = jnp.concatenate(
        [by_column, jnp.broadcast_to(pair_act[None], (columns,) + pair_act.shape)], axis=1
    )
    gathered = lax.all_to_all(payload, "x", split_axis=0, concat_axis=0, tiled=True)
    picked = gathered[:, :slots].reshape(columns, groups, cap, block)
    high = lax.reduce_precision(weight, 8, 7)
    low = weight - high
    routed = jnp.zeros((rows, block), jnp.float32)
    for s in range(cap):
        values = picked[:, :, s].reshape(columns * groups, block)
        here = ahead == s
        for part in (high, low):
            routed = routed + dot(jnp.where(here, part, 0.0).astype(jnp.bfloat16), values)
    act = gathered[:, slots:].reshape(-1, rows)
    shared_out = dot(act, shared_down, ((0,), (0,)))
    return (routed + shared_out).astype(jnp.bfloat16)


def solution(mesh):
    ep = mesh.shape["ep"]
    tp = mesh.shape["tp"]
    finer = Mesh(mesh.devices.reshape(8, ep // 8, tp // 2, 2), ALL)
    in_specs = (
        P(EP, None),
        P(),
        P(EP, None),
        P(EP, None),
        P(ALL, None, None),
        P(ALL, None, None),
        P(ALL, None, None),
        P(None, TP),
        P(None, TP),
        P(None, TP),
    )
    out_specs = P(EP, TP)
    return jax.shard_map(local, mesh=finer, in_specs=in_specs, out_specs=out_specs, check_vma=False)
```

```python
import jax
import jax.numpy as jnp
from jax import lax
from jax.sharding import Mesh
from jax.sharding import PartitionSpec as P

TP = ("x", "core")
EP = ("z", "y")
ALL = ("z", "y", "x", "core")

NORM_EPSILON = 1e-06


def dot(a, b, dims=((1,), (0,))):
    return lax.dot_general(a, b, (dims, ((), ())), preferred_element_type=jnp.float32)


def local(
    tokens,
    norm_gain,
    expert_ids,
    route_weights,
    expert_gate,
    expert_up,
    expert_down,
    shared_gate,
    shared_up,
    shared_down,
):
    groups = lax.axis_size(EP)
    columns = lax.axis_size("x")
    cores = lax.axis_size("core")
    column = lax.axis_index("x")
    core = lax.axis_index("core")
    rows, width = tokens.shape
    top_count = expert_ids.shape[1]
    tp_count = columns * cores
    block = width // tp_count

    as_float = tokens.astype(jnp.float32)
    inverse_rms = lax.rsqrt(jnp.mean(as_float * as_float, axis=-1, keepdims=True) + NORM_EPSILON)
    normed = (as_float * inverse_rms * norm_gain).astype(jnp.bfloat16)

    token_iota = jnp.arange(rows, dtype=jnp.int32)
    strict_lower = (token_iota[:, None] > token_iota[None, :]).astype(jnp.bfloat16)

    own_expert = jnp.arange(groups, dtype=jnp.int32) * columns + column
    own = jnp.zeros((rows, groups), jnp.bool_)
    for k in range(top_count):
        own = own | (expert_ids[:, k : k + 1] == own_expert[None, :])
    before = dot(strict_lower, own.astype(jnp.bfloat16))
    chosen = own & (before == core.astype(jnp.float32))
    buffer = dot(chosen.astype(jnp.bfloat16), normed, ((0,), (0,))).astype(jnp.bfloat16)
    with jax.named_scope("dispatch"):
        received = lax.all_to_all(
            buffer.reshape(groups, tp_count, block), EP, split_axis=0, concat_axis=0, tiled=True
        )

    swap = [(0, 1), (1, 0)]
    with jax.named_scope("weights"):
        gates = [expert_gate[0], lax.ppermute(expert_gate[0], "core", swap)]
        ups = [expert_up[0], lax.ppermute(expert_up[0], "core", swap)]
        downs = [expert_down[0], lax.ppermute(expert_down[0], "core", swap)]

    shared_act = (
        jax.nn.silu(dot(shared_gate, normed, ((0,), (1,)))) * dot(shared_up, normed, ((0,), (1,)))
    ).astype(jnp.bfloat16)

    slot_iota = jnp.arange(tp_count * groups, dtype=jnp.int32)
    slot_expert = (slot_iota % groups) * columns + slot_iota // (groups * cores)
    slot_number = (slot_iota // groups) % cores
    weight = jnp.zeros((rows, tp_count * groups), jnp.float32)
    taken = jnp.zeros((rows, tp_count * groups), jnp.bool_)
    for k in range(top_count):
        hit = expert_ids[:, k : k + 1] == slot_expert[None, :]
        taken = taken | hit
        weight = jnp.where(hit, route_weights[:, k : k + 1], weight)
    ahead = dot(strict_lower, taken.astype(jnp.bfloat16))
    weight = jnp.where(ahead == slot_number.astype(jnp.float32)[None, :], weight, 0.0)
    high = lax.reduce_precision(weight, 8, 7)
    parts = (high.astype(jnp.bfloat16), (weight - high).astype(jnp.bfloat16))

    flat_rows = lax.optimization_barrier(received.reshape(groups, width))
    expert_out = jnp.zeros((groups, width), jnp.float32)
    for gate, up, down in zip(gates, ups, downs):
        hidden = (jax.nn.silu(dot(flat_rows, gate)) * dot(flat_rows, up)).astype(jnp.bfloat16)
        expert_out = expert_out + dot(hidden, down)
    expert_out = expert_out.astype(jnp.bfloat16)
    with jax.named_scope("back"):
        returned = lax.all_to_all(
            expert_out.reshape(groups, tp_count, block), EP, split_axis=0, concat_axis=0, tiled=True
        )
    payload = jnp.concatenate(
        [
            jnp.swapaxes(returned, 0, 1),
            jnp.broadcast_to(shared_act[None], (tp_count,) + shared_act.shape),
        ],
        axis=1,
    )
    payload, *parts = lax.optimization_barrier((payload, *parts))
    with jax.named_scope("share"):
        gathered = lax.all_to_all(payload, TP, split_axis=0, concat_axis=0, tiled=True)
    values = gathered[:, :groups].reshape(tp_count * groups, block)
    act = gathered[:, groups:].reshape(-1, rows)
    mixed = dot(parts[0], values) + dot(parts[1], values) + dot(act, shared_down, ((0,), (0,)))
    return mixed.astype(jnp.bfloat16)


def solution(mesh):
    ep = mesh.shape["ep"]
    tp = mesh.shape["tp"]
    finer = Mesh(mesh.devices.reshape(8, ep // 8, tp // 2, 2), ALL)
    in_specs = (
        P(EP, None),
        P(),
        P(EP, None),
        P(EP, None),
        P(ALL, None, None),
        P(ALL, None, None),
        P(ALL, None, None),
        P(None, TP),
        P(None, TP),
        P(None, TP),
    )
    out_specs = P(EP, TP)
    return jax.shard_map(local, mesh=finer, in_specs=in_specs, out_specs=out_specs, check_vma=False)
```

```python
import jax
import jax.numpy as jnp
from jax import lax
from jax.experimental import pallas as pl
from jax.experimental.pallas import tpu as pltpu
from jax.sharding import Mesh
from jax.sharding import PartitionSpec as P


TP = ("x", "core")
EP = ("z", "y")
ALL = ("z", "y", "x", "core")

NORM_EPSILON = 1e-06
INTERPRET = False


def dot(a, b, dims=((1,), (0,))):
    return lax.dot_general(a, b, (dims, ((), ())), preferred_element_type=jnp.float32)


def pick_rows(place, far_ids, far_tokens, far_gain, out, ids, tokens, gain, sems):
    pairs = ((far_ids, ids), (far_tokens, tokens), (far_gain, gain))
    copies = [pltpu.make_async_copy(*pairs[i], sems.at[i]) for i in range(len(pairs))]
    for copy in copies:
        copy.start()
    columns = place[1]
    column, core = place[0] // place[2], place[0] % place[2]
    top_count, rows = ids.shape
    groups, width = out.shape
    expert = lax.broadcasted_iota(jnp.int32, (groups, rows), 0) * columns + column
    copies[0].wait()
    own = ids[0:1, :] == expert
    for k in range(1, top_count):
        own = own | (ids[k : k + 1, :] == expert)
    own = jnp.where(own, 1.0, 0.0)
    sooner = lax.broadcasted_iota(jnp.int32, (rows, rows), 0) < lax.broadcasted_iota(
        jnp.int32, (rows, rows), 1
    )
    before = dot(own.astype(jnp.bfloat16), jnp.where(sooner, 1.0, 0.0).astype(jnp.bfloat16))
    chosen = jnp.where(before == core.astype(jnp.float32), own, 0.0).astype(jnp.bfloat16)
    copies[1].wait()
    as_float = tokens[...].astype(jnp.float32)
    square = jnp.sum(as_float * as_float, axis=1, keepdims=True) * (1.0 / width)
    copies[2].wait()
    normed = (as_float * lax.rsqrt(square + NORM_EPSILON) * gain[...]).astype(jnp.bfloat16)
    out[...] = dot(chosen, normed).astype(jnp.bfloat16)


def expert_body(x, near, up_a, down_a, gate_b, up_b, down_b, out, wide, tall, sems):
    sources = (up_a, down_a, gate_b, up_b, down_b)
    targets = (wide.at[0], tall.at[0], wide.at[1], wide.at[2], tall.at[1])
    copies = [
        pltpu.make_async_copy(sources[i], targets[i], sems.at[i]) for i in range(len(sources))
    ]
    for copy in copies:
        copy.start()

    def hidden(gated, lifted):
        return (gated / (1.0 + jnp.exp(-gated)) * lifted).astype(jnp.bfloat16)

    gated = dot(x[...], near[...])
    copies[0].wait()
    acts = hidden(gated, dot(x[...], wide[0]))
    copies[1].wait()
    total = dot(acts, tall[0])
    copies[2].wait()
    gated = dot(x[...], wide[1])
    copies[3].wait()
    acts = hidden(gated, dot(x[...], wide[2]))
    copies[4].wait()
    out[...] = (total + dot(acts, tall[1])).astype(jnp.bfloat16)


def finish(gathered, high, low, down, out):
    tp_count = gathered.shape[0]
    groups = high.shape[1] // tp_count
    values = jnp.concatenate([gathered[s, :groups] for s in range(tp_count)], axis=0)
    act = jnp.concatenate([gathered[s, groups:] for s in range(tp_count)], axis=0)
    mixed = dot(high[...], values) + dot(low[...], values)
    out[...] = (mixed + dot(act, down[...], ((0,), (0,)))).astype(jnp.bfloat16)


def in_vmem(body, shape, *args, smem=0, anywhere=(), scratch=(), onward=False):
    specs = []
    args = list(args)
    for i in range(len(args)):
        space = pltpu.SMEM if i < smem else pltpu.HBM if i in anywhere else pltpu.VMEM
        specs.append(pl.BlockSpec(memory_space=space))
        if i >= smem and not INTERPRET:
            args[i] = pltpu.with_memory_space_constraint(args[i], space)
    out = jax.ShapeDtypeStruct(shape, jnp.bfloat16)
    return pl.pallas_call(
        body,
        out_shape=pltpu.VMEM(shape, jnp.bfloat16) if onward and not INTERPRET else out,
        in_specs=specs,
        out_specs=pl.BlockSpec(memory_space=pltpu.VMEM),
        scratch_shapes=list(scratch),
        interpret=INTERPRET,
    )(*args)


def local(
    tokens,
    norm_gain,
    expert_ids,
    route_weights,
    expert_gate,
    expert_up,
    expert_down,
    shared_gate,
    shared_up,
    shared_down,
):
    groups = lax.axis_size(EP)
    columns = lax.axis_size("x")
    cores = lax.axis_size("core")
    rows, width = tokens.shape
    top_count = expert_ids.shape[1]
    tp_count = columns * cores
    block = width // tp_count

    as_float = tokens.astype(jnp.float32)
    inverse_rms = lax.rsqrt(jnp.mean(as_float * as_float, axis=-1, keepdims=True) + NORM_EPSILON)
    normed = (as_float * inverse_rms * norm_gain).astype(jnp.bfloat16)

    token_iota = jnp.arange(rows, dtype=jnp.int32)
    strict_lower = (token_iota[:, None] > token_iota[None, :]).astype(jnp.bfloat16)

    place = jnp.stack([lax.axis_index(TP), jnp.int32(columns), jnp.int32(cores)])
    buffer = in_vmem(
        pick_rows,
        (groups, width),
        place,
        expert_ids.T,
        tokens,
        norm_gain[None],
        smem=1,
        anywhere=range(1, 4),
        onward=True,
        scratch=(
            pltpu.VMEM((top_count, rows), jnp.int32),
            pltpu.VMEM((rows, width), jnp.bfloat16),
            pltpu.VMEM((1, width), jnp.float32),
            pltpu.SemaphoreType.DMA((3,)),
        ),
    )
    received = lax.all_to_all(
        buffer.reshape(groups, tp_count, block), EP, split_axis=0, concat_axis=0, tiled=True
    )

    swap = [(0, 1), (1, 0)]
    halves = []
    for half in (expert_gate, expert_up, expert_down):
        halves.append((half[0], lax.ppermute(half[0], "core", swap)))
    gates, ups, downs = halves

    shared_act = (
        jax.nn.silu(dot(shared_gate, normed, ((0,), (1,)))) * dot(shared_up, normed, ((0,), (1,)))
    ).astype(jnp.bfloat16)

    slot_iota = jnp.arange(tp_count * groups, dtype=jnp.int32)
    slot_expert = (slot_iota % groups) * columns + slot_iota // (groups * cores)
    slot_number = (slot_iota // groups) % cores
    weight = jnp.zeros((rows, tp_count * groups), jnp.float32)
    taken = jnp.zeros((rows, tp_count * groups), jnp.bool_)
    for k in range(top_count):
        hit = expert_ids[:, k : k + 1] == slot_expert[None, :]
        taken = taken | hit
        weight = jnp.where(hit, route_weights[:, k : k + 1], weight)
    ahead = dot(strict_lower, taken.astype(jnp.bfloat16))
    weight = jnp.where(ahead == slot_number.astype(jnp.float32)[None, :], weight, 0.0)
    high = lax.reduce_precision(weight, 8, 7)
    parts = (high.astype(jnp.bfloat16), (weight - high).astype(jnp.bfloat16))

    inner = expert_gate.shape[2]
    expert_out = in_vmem(
        expert_body,
        (groups, width),
        received.reshape(groups, width),
        gates[1],
        ups[1],
        downs[1],
        gates[0],
        ups[0],
        downs[0],
        anywhere=range(2, 7),
        onward=True,
        scratch=(
            pltpu.VMEM((3, width, inner), jnp.bfloat16),
            pltpu.VMEM((2, inner, width), jnp.bfloat16),
            pltpu.SemaphoreType.DMA((5,)),
        ),
    )
    returned = lax.all_to_all(
        expert_out.reshape(groups, tp_count, block), EP, split_axis=0, concat_axis=0, tiled=True
    )
    payload = jnp.concatenate(
        [
            jnp.swapaxes(returned, 0, 1),
            jnp.broadcast_to(shared_act[None], (tp_count,) + shared_act.shape),
        ],
        axis=1,
    )
    payload, *parts = lax.optimization_barrier((payload, *parts))
    gathered = lax.all_to_all(payload, TP, split_axis=0, concat_axis=0, tiled=True)
    return in_vmem(finish, (rows, block), gathered, *parts, shared_down)


def solution(mesh):
    ep = mesh.shape["ep"]
    tp = mesh.shape["tp"]
    finer = Mesh(mesh.devices.reshape(8, ep // 8, tp // 2, 2), ALL)
    in_specs = (
        P(EP, None),
        P(),
        P(EP, None),
        P(EP, None),
        P(ALL, None, None),
        P(ALL, None, None),
        P(ALL, None, None),
        P(None, TP),
        P(None, TP),
        P(None, TP),
    )
    out_specs = P(EP, TP)

    return jax.shard_map(local, mesh=finer, in_specs=in_specs, out_specs=out_specs, check_vma=False)
```

```python
import functools

import jax
import jax.numpy as jnp
from jax import lax
from jax.experimental import pallas as pl
from jax.experimental.pallas import tpu as pltpu
from jax.sharding import Mesh
from jax.sharding import PartitionSpec as P


TP = ("x", "core")
EP = ("z", "y")
ALL = ("z", "y", "x", "core")

NORM_EPSILON = 1e-06
INTERPRET = False


def dot(a, b, dims=((1,), (0,))):
    return lax.dot_general(a, b, (dims, ((), ())), preferred_element_type=jnp.float32)


def row_major(value, scratch, out):
    rows, width = value.shape
    block = out.shape[1]
    count = width // block
    for b in range(count):
        scratch[pl.ds(b, rows, stride=count), :] = value[:, b * block : (b + 1) * block]
    out[...] = scratch[...].astype(jnp.bfloat16)


def pick_rows(columns, cores, place, far_ids, far_tokens, far_gain, out, ids, tokens, gain, wide, sems):
    pairs = ((far_ids, ids), (far_tokens, tokens), (far_gain, gain))
    copies = [pltpu.make_async_copy(*pairs[i], sems.at[i]) for i in range(len(pairs))]
    for copy in copies:
        copy.start()
    column, core = place[0] // cores, place[0] % cores
    top_count, rows = ids.shape
    width = tokens.shape[1]
    groups = out.shape[0] * out.shape[1] // width
    expert = lax.broadcasted_iota(jnp.int32, (groups, rows), 0) * columns + column
    copies[0].wait()
    own = ids[0:1, :] == expert
    for k in range(1, top_count):
        own = own | (ids[k : k + 1, :] == expert)
    own = jnp.where(own, 1.0, 0.0)
    sooner = lax.broadcasted_iota(jnp.int32, (rows, rows), 0) < lax.broadcasted_iota(
        jnp.int32, (rows, rows), 1
    )
    before = dot(own.astype(jnp.bfloat16), jnp.where(sooner, 1.0, 0.0).astype(jnp.bfloat16))
    chosen = jnp.where(before == core.astype(jnp.float32), own, 0.0).astype(jnp.bfloat16)
    copies[1].wait()
    as_float = tokens[...].astype(jnp.float32)
    square = jnp.sum(as_float * as_float, axis=1, keepdims=True) * (1.0 / width)
    copies[2].wait()
    normed = (as_float * lax.rsqrt(square + NORM_EPSILON) * gain[...]).astype(jnp.bfloat16)
    row_major(dot(chosen, normed), wide, out)


def expert_body(x, near, up_a, down_a, gate_b, up_b, down_b, out, wide, tall, flat, sems):
    sources = (up_a, down_a, gate_b, up_b, down_b)
    targets = (wide.at[0], tall.at[0], wide.at[1], wide.at[2], tall.at[1])
    copies = [
        pltpu.make_async_copy(sources[i], targets[i], sems.at[i]) for i in range(len(sources))
    ]
    for copy in copies:
        copy.start()

    def hidden(gated, lifted):
        return (gated / (1.0 + jnp.exp(-gated)) * lifted).astype(jnp.bfloat16)

    gated = dot(x[...], near[...])
    copies[0].wait()
    acts = hidden(gated, dot(x[...], wide[0]))
    copies[1].wait()
    total = dot(acts, tall[0])
    copies[2].wait()
    gated = dot(x[...], wide[1])
    copies[3].wait()
    acts = hidden(gated, dot(x[...], wide[2]))
    copies[4].wait()
    row_major(total + dot(acts, tall[1]), flat, out)


def finish(gathered, high, low, down, out):
    tp_count = gathered.shape[0]
    groups = high.shape[1] // tp_count
    values = jnp.concatenate([gathered[s, :groups] for s in range(tp_count)], axis=0)
    act = jnp.concatenate([gathered[s, groups:] for s in range(tp_count)], axis=0)
    mixed = dot(high[...], values) + dot(low[...], values)
    out[...] = (mixed + dot(act, down[...], ((0,), (0,)))).astype(jnp.bfloat16)


def in_vmem(body, shape, *args, smem=0, anywhere=(), scratch=(), onward=False):
    specs = []
    args = list(args)
    for i in range(len(args)):
        space = pltpu.SMEM if i < smem else pltpu.HBM if i in anywhere else pltpu.VMEM
        specs.append(pl.BlockSpec(memory_space=space))
        if i >= smem and not INTERPRET:
            args[i] = pltpu.with_memory_space_constraint(args[i], space)
    out = jax.ShapeDtypeStruct(shape, jnp.bfloat16)
    return pl.pallas_call(
        body,
        out_shape=pltpu.VMEM(shape, jnp.bfloat16) if onward and not INTERPRET else out,
        in_specs=specs,
        out_specs=pl.BlockSpec(memory_space=pltpu.VMEM),
        scratch_shapes=list(scratch),
        interpret=INTERPRET,
    )(*args)


def late_work(tokens, norm_gain, expert_ids, route_weights, shared_gate, shared_up, groups):
    columns = lax.axis_size("x")
    cores = lax.axis_size("core")
    tp_count = columns * cores
    rows, top_count = expert_ids.shape
    as_float = tokens.astype(jnp.float32)
    inverse_rms = lax.rsqrt(jnp.mean(as_float * as_float, axis=-1, keepdims=True) + NORM_EPSILON)
    normed = (as_float * inverse_rms * norm_gain).astype(jnp.bfloat16)

    shared_act = (
        jax.nn.silu(dot(shared_gate, normed, ((0,), (1,)))) * dot(shared_up, normed, ((0,), (1,)))
    ).astype(jnp.bfloat16)

    token_iota = jnp.arange(rows, dtype=jnp.int32)
    strict_lower = (token_iota[:, None] > token_iota[None, :]).astype(jnp.bfloat16)

    slot_iota = jnp.arange(tp_count * groups, dtype=jnp.int32)
    slot_expert = (slot_iota % groups) * columns + slot_iota // (groups * cores)
    slot_number = (slot_iota // groups) % cores
    weight = jnp.zeros((rows, tp_count * groups), jnp.float32)
    taken = jnp.zeros((rows, tp_count * groups), jnp.bool_)
    for k in range(top_count):
        hit = expert_ids[:, k : k + 1] == slot_expert[None, :]
        taken = taken | hit
        weight = jnp.where(hit, route_weights[:, k : k + 1], weight)
    ahead = dot(strict_lower, taken.astype(jnp.bfloat16))
    weight = jnp.where(ahead == slot_number.astype(jnp.float32)[None, :], weight, 0.0)
    high = lax.reduce_precision(weight, 8, 7)
    parts = (high.astype(jnp.bfloat16), (weight - high).astype(jnp.bfloat16))
    return shared_act, parts


def local(
    tokens,
    norm_gain,
    expert_ids,
    route_weights,
    expert_gate,
    expert_up,
    expert_down,
    shared_gate,
    shared_up,
    shared_down,
):
    groups = lax.axis_size(EP)
    columns = lax.axis_size("x")
    cores = lax.axis_size("core")
    rows, width = tokens.shape
    top_count = expert_ids.shape[1]
    tp_count = columns * cores
    block = width // tp_count

    flat = (groups * tp_count, block)
    buffer = in_vmem(
        functools.partial(pick_rows, columns, cores),
        flat,
        lax.axis_index(TP)[None],
        expert_ids.T,
        tokens,
        norm_gain[None],
        smem=1,
        anywhere=range(1, 4),
        onward=True,
        scratch=(
            pltpu.VMEM((top_count, rows), jnp.int32),
            pltpu.VMEM((rows, width), jnp.bfloat16),
            pltpu.VMEM((1, width), jnp.float32),
            pltpu.VMEM(flat, jnp.float32),
            pltpu.SemaphoreType.DMA((3,)),
        ),
    )
    received = lax.all_to_all(
        buffer.reshape(groups, tp_count, block), EP, split_axis=0, concat_axis=0, tiled=True
    )

    swap = [(0, 1), (1, 0)]
    halves = []
    for half in (expert_gate, expert_up, expert_down):
        halves.append((half[0], lax.ppermute(half[0], "core", swap)))
    gates, ups, downs = halves

    inner = expert_gate.shape[2]
    expert_out = in_vmem(
        expert_body,
        flat,
        received.reshape(groups, width),
        gates[1],
        ups[1],
        downs[1],
        gates[0],
        ups[0],
        downs[0],
        anywhere=range(2, 7),
        onward=True,
        scratch=(
            pltpu.VMEM((3, width, inner), jnp.bfloat16),
            pltpu.VMEM((2, inner, width), jnp.bfloat16),
            pltpu.VMEM(flat, jnp.float32),
            pltpu.SemaphoreType.DMA((5,)),
        ),
    )
    returned = lax.all_to_all(
        expert_out.reshape(groups, tp_count, block), EP, split_axis=0, concat_axis=0, tiled=True
    )
    shared_act, parts = late_work(
        tokens, norm_gain, expert_ids, route_weights, shared_gate, shared_up, groups
    )
    payload = jnp.concatenate(
        [
            jnp.swapaxes(returned, 0, 1),
            jnp.broadcast_to(shared_act[None], (tp_count,) + shared_act.shape),
        ],
        axis=1,
    )
    payload, *parts = lax.optimization_barrier((payload, *parts))
    gathered = lax.all_to_all(payload, TP, split_axis=0, concat_axis=0, tiled=True)
    return in_vmem(finish, (rows, block), gathered, *parts, shared_down)


def solution(mesh):
    ep = mesh.shape["ep"]
    tp = mesh.shape["tp"]
    finer = Mesh(mesh.devices.reshape(8, ep // 8, tp // 2, 2), ALL)
    in_specs = (
        P(EP, None),
        P(),
        P(EP, None),
        P(EP, None),
        P(ALL, None, None),
        P(ALL, None, None),
        P(ALL, None, None),
        P(None, TP),
        P(None, TP),
        P(None, TP),
    )
    out_specs = P(EP, TP)

    return jax.shard_map(local, mesh=finer, in_specs=in_specs, out_specs=out_specs, check_vma=False)
```

```python
import functools

import jax
import jax.numpy as jnp
from jax import lax
from jax.experimental import pallas as pl
from jax.experimental.pallas import tpu as pltpu
from jax.sharding import Mesh
from jax.sharding import PartitionSpec as P


TP = ("x", "core")
EP = ("z", "y")
ALL = ("z", "y", "x", "core")

NORM_EPSILON = 1e-06
INTERPRET = False


def dot(a, b, dims=((1,), (0,))):
    return lax.dot_general(a, b, (dims, ((), ())), preferred_element_type=jnp.float32)


def row_major(piece, width, scratch, out):
    block = out.shape[1]
    count = width // block
    rows = out.shape[0] // count
    for first in range(0, count, 2):
        value = piece(slice(first * block, (first + 2) * block))
        for b in range(2):
            here = value[:, b * block : (b + 1) * block]
            scratch[pl.ds(first + b, rows, stride=count), :] = here
    out[...] = scratch[...].astype(jnp.bfloat16)


def pick_rows(columns, cores, place, far_ids, far_tokens, far_gain, out, ids, tokens, gain, wide, sems):
    pairs = ((far_ids, ids), (far_tokens, tokens), (far_gain, gain))
    copies = [pltpu.make_async_copy(*pairs[i], sems.at[i]) for i in range(len(pairs))]
    for copy in copies:
        copy.start()
    column, core = place[0] // cores, place[0] % cores
    top_count, rows = ids.shape
    width = tokens.shape[1]
    groups = out.shape[0] * out.shape[1] // width
    expert = lax.broadcasted_iota(jnp.int32, (groups, rows), 0) * columns + column
    copies[0].wait()
    own = ids[0:1, :] == expert
    for k in range(1, top_count):
        own = own | (ids[k : k + 1, :] == expert)
    own = jnp.where(own, 1.0, 0.0)
    sooner = lax.broadcasted_iota(jnp.int32, (rows, rows), 0) < lax.broadcasted_iota(
        jnp.int32, (rows, rows), 1
    )
    before = dot(own.astype(jnp.bfloat16), jnp.where(sooner, 1.0, 0.0).astype(jnp.bfloat16))
    chosen = jnp.where(before == core.astype(jnp.float32), own, 0.0).astype(jnp.bfloat16)
    copies[1].wait()
    as_float = tokens[...].astype(jnp.float32)
    square = jnp.sum(as_float * as_float, axis=1, keepdims=True) * (1.0 / width)
    copies[2].wait()
    normed = (as_float * lax.rsqrt(square + NORM_EPSILON) * gain[...]).astype(jnp.bfloat16)
    row_major(lambda span: dot(chosen, normed[:, span]), width, wide, out)


def hidden_units(x, gate_a, up_a, gate_b, up_b, out, wide, sems):
    sources = (up_a, gate_b, up_b)
    copies = [
        pltpu.make_async_copy(sources[i], wide.at[i], sems.at[i]) for i in range(len(sources))
    ]
    for copy in copies:
        copy.start()
    inner = wide.shape[2]

    def acts(gated, lifted):
        return (gated / (1.0 + jnp.exp(-gated)) * lifted).astype(jnp.bfloat16)

    gated = dot(x[...], gate_a[...])
    copies[0].wait()
    out[:, inner:] = acts(gated, dot(x[...], wide[0]))
    copies[1].wait()
    gated = dot(x[...], wide[1])
    copies[2].wait()
    out[:, :inner] = acts(gated, dot(x[...], wide[2]))


def products(acts, down_a, down_b, out, flat):
    inner = down_a.shape[0]

    def piece(span):
        return dot(acts[:, :inner], down_b[:, span]) + dot(acts[:, inner:], down_a[:, span])

    row_major(piece, down_a.shape[1], flat, out)


def finish(gathered, high, low, down, out):
    tp_count = gathered.shape[0]
    groups = high.shape[1] // tp_count
    values = jnp.concatenate([gathered[s, :groups] for s in range(tp_count)], axis=0)
    act = jnp.concatenate([gathered[s, groups:] for s in range(tp_count)], axis=0)
    mixed = dot(jnp.concatenate([high[...], low[...]], axis=0), values)
    mixed = mixed[: high.shape[0]] + mixed[high.shape[0] :]
    out[...] = (mixed + dot(act, down[...], ((0,), (0,)))).astype(jnp.bfloat16)


def in_vmem(body, shape, *args, smem=0, anywhere=(), scratch=(), onward=False, room=12):
    specs = []
    args = list(args)
    for i in range(len(args)):
        space = pltpu.SMEM if i < smem else pltpu.HBM if i in anywhere else pltpu.VMEM
        specs.append(pl.BlockSpec(memory_space=space))
        if i >= smem and not INTERPRET:
            args[i] = pltpu.with_memory_space_constraint(args[i], space)
    out = jax.ShapeDtypeStruct(shape, jnp.bfloat16)
    return pl.pallas_call(
        body,
        out_shape=pltpu.VMEM(shape, jnp.bfloat16) if onward and not INTERPRET else out,
        in_specs=specs,
        out_specs=pl.BlockSpec(memory_space=pltpu.VMEM),
        scratch_shapes=list(scratch),
        interpret=INTERPRET,
        compiler_params=pltpu.CompilerParams(vmem_limit_bytes=room << 20),
    )(*args)


def late_work(tokens, norm_gain, expert_ids, route_weights, shared_gate, shared_up, groups):
    columns = lax.axis_size("x")
    cores = lax.axis_size("core")
    tp_count = columns * cores
    rows, top_count = expert_ids.shape
    as_float = tokens.astype(jnp.float32)
    inverse_rms = lax.rsqrt(jnp.mean(as_float * as_float, axis=-1, keepdims=True) + NORM_EPSILON)
    normed = (as_float * inverse_rms * norm_gain).astype(jnp.bfloat16)

    shared_act = (
        jax.nn.silu(dot(shared_gate, normed, ((0,), (1,)))) * dot(shared_up, normed, ((0,), (1,)))
    ).astype(jnp.bfloat16)

    token_iota = jnp.arange(rows, dtype=jnp.int32)
    strict_lower = (token_iota[:, None] > token_iota[None, :]).astype(jnp.bfloat16)

    slot_iota = jnp.arange(tp_count * groups, dtype=jnp.int32)
    slot_expert = (slot_iota % groups) * columns + slot_iota // (groups * cores)
    slot_number = (slot_iota // groups) % cores
    weight = jnp.zeros((rows, tp_count * groups), jnp.float32)
    taken = jnp.zeros((rows, tp_count * groups), jnp.bool_)
    for k in range(top_count):
        hit = expert_ids[:, k : k + 1] == slot_expert[None, :]
        taken = taken | hit
        weight = jnp.where(hit, route_weights[:, k : k + 1], weight)
    ahead = dot(strict_lower, taken.astype(jnp.bfloat16))
    weight = jnp.where(ahead == slot_number.astype(jnp.float32)[None, :], weight, 0.0)
    high = lax.reduce_precision(weight, 8, 7)
    parts = (high.astype(jnp.bfloat16), (weight - high).astype(jnp.bfloat16))
    return shared_act, parts


def local(
    tokens,
    norm_gain,
    expert_ids,
    route_weights,
    expert_gate,
    expert_up,
    expert_down,
    shared_gate,
    shared_up,
    shared_down,
):
    groups = lax.axis_size(EP)
    columns = lax.axis_size("x")
    cores = lax.axis_size("core")
    rows, width = tokens.shape
    top_count = expert_ids.shape[1]
    tp_count = columns * cores
    block = width // tp_count

    flat = (groups * tp_count, block)
    buffer = in_vmem(
        functools.partial(pick_rows, columns, cores),
        flat,
        lax.axis_index(TP)[None],
        expert_ids.T,
        tokens,
        norm_gain[None],
        smem=1,
        anywhere=range(1, 4),
        onward=True,
        scratch=(
            pltpu.VMEM((top_count, rows), jnp.int32),
            pltpu.VMEM((rows, width), jnp.bfloat16),
            pltpu.VMEM((1, width), jnp.float32),
            pltpu.VMEM(flat, jnp.float32),
            pltpu.SemaphoreType.DMA((3,)),
        ),
    )
    received = lax.all_to_all(
        buffer.reshape(groups, tp_count, block), EP, split_axis=0, concat_axis=0, tiled=True
    )

    swap = [(0, 1), (1, 0)]
    halves = []
    for half in (expert_gate, expert_up, expert_down):
        halves.append((half[0], lax.ppermute(half[0], "core", swap)))
    gates, ups, downs = halves

    inner = expert_gate.shape[2]
    acts = in_vmem(
        hidden_units,
        (groups, 2 * inner),
        received.reshape(groups, width),
        gates[1],
        ups[1],
        gates[0],
        ups[0],
        anywhere=range(2, 5),
        onward=True,
        scratch=(pltpu.VMEM((3, width, inner), jnp.bfloat16), pltpu.SemaphoreType.DMA((3,))),
    )
    expert_out = in_vmem(
        products,
        flat,
        acts,
        downs[1],
        downs[0],
        onward=True,
        scratch=(pltpu.VMEM(flat, jnp.float32),),
    )
    returned = lax.all_to_all(
        expert_out.reshape(groups, tp_count, block), EP, split_axis=0, concat_axis=0, tiled=True
    )
    shared_act, parts = late_work(
        tokens, norm_gain, expert_ids, route_weights, shared_gate, shared_up, groups
    )
    payload = jnp.concatenate(
        [
            jnp.swapaxes(returned, 0, 1),
            jnp.broadcast_to(shared_act[None], (tp_count,) + shared_act.shape),
        ],
        axis=1,
    )
    payload, *parts = lax.optimization_barrier((payload, *parts))
    gathered = lax.all_to_all(payload, TP, split_axis=0, concat_axis=0, tiled=True)
    return in_vmem(finish, (rows, block), gathered, *parts, shared_down)


def solution(mesh):
    ep = mesh.shape["ep"]
    tp = mesh.shape["tp"]
    finer = Mesh(mesh.devices.reshape(8, ep // 8, tp // 2, 2), ALL)
    in_specs = (
        P(EP, None),
        P(),
        P(EP, None),
        P(EP, None),
        P(ALL, None, None),
        P(ALL, None, None),
        P(ALL, None, None),
        P(None, TP),
        P(None, TP),
        P(None, TP),
    )
    out_specs = P(EP, TP)

    return jax.shard_map(local, mesh=finer, in_specs=in_specs, out_specs=out_specs, check_vma=False)
```

```python
import functools

import jax
import jax.numpy as jnp
from jax import lax
from jax.experimental import pallas as pl
from jax.experimental.pallas import tpu as pltpu
from jax.sharding import Mesh
from jax.sharding import PartitionSpec as P


TP = ("x", "core")
EP = ("z", "y")
ALL = ("z", "y", "x", "core")

NORM_EPSILON = 1e-06
INTERPRET = False


def dot(a, b, dims=((1,), (0,))):
    return lax.dot_general(a, b, (dims, ((), ())), preferred_element_type=jnp.float32)


def row_major(piece, width, scratch, out):
    block = out.shape[1]
    count = width // block
    rows = out.shape[0] // count
    for first in range(0, count, 2):
        value = piece(slice(first * block, (first + 2) * block))
        for b in range(2):
            here = value[:, b * block : (b + 1) * block]
            scratch[pl.ds(first + b, rows, stride=count), :] = here
    out[...] = scratch[...].astype(jnp.bfloat16)


def pick_rows(columns, cores, place, far_ids, far_tokens, far_gain, out, ids, tokens, gain, wide, sems):
    pairs = ((far_ids, ids), (far_tokens, tokens), (far_gain, gain))
    copies = [pltpu.make_async_copy(*pairs[i], sems.at[i]) for i in range(len(pairs))]
    for copy in copies:
        copy.start()
    column, core = place[0] // cores, place[0] % cores
    top_count, rows = ids.shape
    width = tokens.shape[1]
    groups = out.shape[0] * out.shape[1] // width
    expert = lax.broadcasted_iota(jnp.int32, (groups, rows), 0) * columns + column
    copies[0].wait()
    own = ids[0:1, :] == expert
    for k in range(1, top_count):
        own = own | (ids[k : k + 1, :] == expert)
    own = jnp.where(own, 1.0, 0.0)
    sooner = lax.broadcasted_iota(jnp.int32, (rows, rows), 0) < lax.broadcasted_iota(
        jnp.int32, (rows, rows), 1
    )
    before = dot(own.astype(jnp.bfloat16), jnp.where(sooner, 1.0, 0.0).astype(jnp.bfloat16))
    chosen = jnp.where(before == core.astype(jnp.float32), own, 0.0).astype(jnp.bfloat16)
    copies[1].wait()
    as_float = tokens[...].astype(jnp.float32)
    square = jnp.sum(as_float * as_float, axis=1, keepdims=True) * (1.0 / width)
    copies[2].wait()
    normed = (as_float * lax.rsqrt(square + NORM_EPSILON) * gain[...]).astype(jnp.bfloat16)
    row_major(lambda span: dot(chosen, normed[:, span]), width, wide, out)


def hidden_units(x, gate_a, up_a, gate_b, up_b, out, wide, sems):
    sources = (up_a, gate_b, up_b)
    copies = [
        pltpu.make_async_copy(sources[i], wide.at[i], sems.at[i]) for i in range(len(sources))
    ]
    for copy in copies:
        copy.start()
    inner = wide.shape[2]

    def acts(gated, lifted):
        return (gated / (1.0 + jnp.exp(-gated)) * lifted).astype(jnp.bfloat16)

    gated = dot(x[...], gate_a[...])
    copies[0].wait()
    out[:, inner:] = acts(gated, dot(x[...], wide[0]))
    copies[1].wait()
    gated = dot(x[...], wide[1])
    copies[2].wait()
    out[:, :inner] = acts(gated, dot(x[...], wide[2]))


def products(acts, down_a, down_b, out, flat):
    inner = down_a.shape[0]

    def piece(span):
        return dot(acts[:, :inner], down_b[:, span]) + dot(acts[:, inner:], down_a[:, span])

    row_major(piece, down_a.shape[1], flat, out)


def share(partner, place, gathered, high, low, down, out):
    core = place[0]
    half = 1 - core if partner else core
    columns = gathered.shape[0]
    groups = high.shape[1] // columns
    here = pl.ds(pl.multiple_of(half * groups, groups), groups)
    values = jnp.concatenate([gathered[c, here] for c in range(columns)], axis=0)
    act = jnp.concatenate([gathered[c, 2 * groups :] for c in range(columns)], axis=0)
    mixed = dot(jnp.concatenate([high[...], low[...]], axis=0), values)
    mixed = mixed[: high.shape[0]] + mixed[high.shape[0] :]
    out[...] = mixed + dot(act, down[...], ((0,), (0,)))


def in_vmem(body, shape, *args, dtype=jnp.bfloat16, smem=0, anywhere=(), scratch=(), onward=False, room=12):
    specs = []
    args = list(args)
    for i in range(len(args)):
        space = pltpu.SMEM if i < smem else pltpu.HBM if i in anywhere else pltpu.VMEM
        specs.append(pl.BlockSpec(memory_space=space))
        if i >= smem and not INTERPRET:
            args[i] = pltpu.with_memory_space_constraint(args[i], space)
    out = jax.ShapeDtypeStruct(shape, dtype)
    return pl.pallas_call(
        body,
        out_shape=pltpu.VMEM(shape, dtype) if onward and not INTERPRET else out,
        in_specs=specs,
        out_specs=pl.BlockSpec(memory_space=pltpu.VMEM),
        scratch_shapes=list(scratch),
        interpret=INTERPRET,
        compiler_params=pltpu.CompilerParams(vmem_limit_bytes=room << 20),
    )(*args)


def late_work(tokens, norm_gain, expert_ids, route_weights, shared_gate, shared_up, groups):
    columns = lax.axis_size("x")
    rows, top_count = expert_ids.shape
    as_float = tokens.astype(jnp.float32)
    inverse_rms = lax.rsqrt(jnp.mean(as_float * as_float, axis=-1, keepdims=True) + NORM_EPSILON)
    normed = (as_float * inverse_rms * norm_gain).astype(jnp.bfloat16)

    shared_act = (
        jax.nn.silu(dot(shared_gate, normed, ((0,), (1,)))) * dot(shared_up, normed, ((0,), (1,)))
    ).astype(jnp.bfloat16)

    token_iota = jnp.arange(rows, dtype=jnp.int32)
    strict_lower = (token_iota[:, None] > token_iota[None, :]).astype(jnp.bfloat16)

    slot_iota = jnp.arange(columns * groups, dtype=jnp.int32)
    slot_expert = (slot_iota % groups) * columns + slot_iota // groups
    slot_number = lax.axis_index("core").astype(jnp.float32)
    weight = jnp.zeros((rows, columns * groups), jnp.float32)
    taken = jnp.zeros((rows, columns * groups), jnp.bool_)
    for k in range(top_count):
        hit = expert_ids[:, k : k + 1] == slot_expert[None, :]
        taken = taken | hit
        weight = jnp.where(hit, route_weights[:, k : k + 1], weight)
    ahead = dot(strict_lower, taken.astype(jnp.bfloat16))
    weight = jnp.where(ahead == slot_number, weight, 0.0)
    high = lax.reduce_precision(weight, 8, 7)
    parts = (high.astype(jnp.bfloat16), (weight - high).astype(jnp.bfloat16))
    return shared_act, parts


def local(
    tokens,
    norm_gain,
    expert_ids,
    route_weights,
    expert_gate,
    expert_up,
    expert_down,
    shared_gate,
    shared_up,
    shared_down,
):
    groups = lax.axis_size(EP)
    columns = lax.axis_size("x")
    cores = lax.axis_size("core")
    core = lax.axis_index("core")
    rows, width = tokens.shape
    top_count = expert_ids.shape[1]
    tp_count = columns * cores
    block = width // tp_count

    flat = (groups * tp_count, block)
    buffer = in_vmem(
        functools.partial(pick_rows, columns, cores),
        flat,
        lax.axis_index(TP)[None],
        expert_ids.T,
        tokens,
        norm_gain[None],
        smem=1,
        anywhere=range(1, 4),
        onward=True,
        scratch=(
            pltpu.VMEM((top_count, rows), jnp.int32),
            pltpu.VMEM((rows, width), jnp.bfloat16),
            pltpu.VMEM((1, width), jnp.float32),
            pltpu.VMEM(flat, jnp.float32),
            pltpu.SemaphoreType.DMA((3,)),
        ),
    )
    received = lax.all_to_all(
        buffer.reshape(groups, tp_count, block), EP, split_axis=0, concat_axis=0, tiled=True
    )

    swap = [(0, 1), (1, 0)]
    halves = []
    for half in (expert_gate, expert_up, expert_down):
        halves.append((half[0], lax.ppermute(half[0], "core", swap)))
    gates, ups, downs = halves

    inner = expert_gate.shape[2]
    acts = in_vmem(
        hidden_units,
        (groups, 2 * inner),
        received.reshape(groups, width),
        gates[1],
        ups[1],
        gates[0],
        ups[0],
        anywhere=range(2, 5),
        onward=True,
        scratch=(pltpu.VMEM((3, width, inner), jnp.bfloat16), pltpu.SemaphoreType.DMA((3,))),
    )
    expert_out = in_vmem(
        products,
        flat,
        acts,
        downs[1],
        downs[0],
        onward=True,
        scratch=(pltpu.VMEM(flat, jnp.float32),),
    )
    returned = lax.all_to_all(
        expert_out.reshape(groups, tp_count, block), EP, split_axis=0, concat_axis=0, tiled=True
    )
    shared_act, parts = late_work(
        tokens, norm_gain, expert_ids, route_weights, shared_gate, shared_up, groups
    )
    by_core = shared_down.reshape(columns, cores, -1, block)
    down_own, down_lent = (
        lax.dynamic_index_in_dim(by_core, half, 1, keepdims=False).reshape(-1, block)
        for half in (core, 1 - core)
    )
    down_borrowed = lax.ppermute(down_lent, "core", swap)

    payload = jnp.concatenate(
        [
            jnp.swapaxes(returned, 0, 1).reshape(columns, cores * groups, block),
            jnp.broadcast_to(shared_act[None], (columns,) + shared_act.shape),
        ],
        axis=1,
    )
    payload, down_borrowed, *parts = lax.optimization_barrier((payload, down_borrowed, *parts))
    gathered = lax.all_to_all(payload, "x", split_axis=0, concat_axis=0, tiled=True)
    place = core[None]
    halves = []
    for partner, down in ((True, down_borrowed), (False, down_own)):
        halves.append(
            in_vmem(
                functools.partial(share, partner),
                (rows, block),
                place,
                gathered,
                *parts,
                down,
                dtype=jnp.float32,
                smem=1,
                onward=True,
            )
        )
    from_partner = lax.ppermute(halves[0], "core", swap)
    return (halves[1] + from_partner).astype(jnp.bfloat16)


def solution(mesh):
    ep = mesh.shape["ep"]
    tp = mesh.shape["tp"]
    finer = Mesh(mesh.devices.reshape(8, ep // 8, tp // 2, 2), ALL)
    in_specs = (
        P(EP, None),
        P(),
        P(EP, None),
        P(EP, None),
        P(ALL, None, None),
        P(ALL, None, None),
        P(ALL, None, None),
        P(None, TP),
        P(None, TP),
        P(None, TP),
    )
    out_specs = P(EP, TP)

    return jax.shard_map(local, mesh=finer, in_specs=in_specs, out_specs=out_specs, check_vma=False)
```

```python
import functools

import jax
import jax.numpy as jnp
from jax import lax
from jax.experimental import pallas as pl
from jax.experimental.pallas import tpu as pltpu
from jax.sharding import Mesh
from jax.sharding import PartitionSpec as P


TP = ("x", "core")
EP = ("z", "y")
ALL = ("z", "y", "x", "core")

NORM_EPSILON = 1e-06
INTERPRET = False


def dot(a, b, dims=((1,), (0,))):
    return lax.dot_general(a, b, (dims, ((), ())), preferred_element_type=jnp.float32)


def row_major(piece, width, scratch, out):
    block = out.shape[1]
    count = width // block
    rows = out.shape[0] // count
    for first in range(0, count, 2):
        value = piece(slice(first * block, (first + 2) * block))
        for b in range(2):
            here = value[:, b * block : (b + 1) * block]
            scratch[pl.ds(first + b, rows, stride=count), :] = here
    out[...] = scratch[...].astype(jnp.bfloat16)


def pick_rows(columns, cores, place, far_ids, far_tokens, far_gain, out, ids, tokens, gain, picked, wide, sems):
    pairs = ((far_ids, ids), (far_tokens, tokens), (far_gain, gain))
    copies = [pltpu.make_async_copy(*pairs[i], sems.at[i]) for i in range(len(pairs))]
    for copy in copies:
        copy.start()
    column, core = place[0] // cores, place[0] % cores
    top_count, rows = ids.shape
    width = tokens.shape[1]
    groups = out.shape[0] * out.shape[1] // width
    expert = lax.broadcasted_iota(jnp.int32, (groups, rows), 0) * columns + column
    copies[0].wait()
    own = ids[0:1, :] == expert
    for k in range(1, top_count):
        own = own | (ids[k : k + 1, :] == expert)
    own = jnp.where(own, 1.0, 0.0)
    sooner = lax.broadcasted_iota(jnp.int32, (rows, rows), 0) < lax.broadcasted_iota(
        jnp.int32, (rows, rows), 1
    )
    before = dot(own.astype(jnp.bfloat16), jnp.where(sooner, 1.0, 0.0).astype(jnp.bfloat16))
    chosen = jnp.where(before == core.astype(jnp.float32), own, 0.0).astype(jnp.bfloat16)
    copies[1].wait()
    step = 2 * out.shape[1]
    spans = [slice(first, first + step) for first in range(0, width, step)]
    squares = jnp.zeros((groups, step), jnp.float32)
    for span in spans:
        row = dot(chosen, tokens[:, span])
        picked[:, span] = row
        squares = squares + row * row
    mean = jnp.sum(squares, axis=1, keepdims=True) * (1.0 / width)
    scale = lax.rsqrt(mean + NORM_EPSILON)
    copies[2].wait()
    row_major(lambda span: picked[:, span] * scale * gain[:, span], width, wide, out)


def hidden_units(x, gate_a, up_a, gate_b, up_b, down_b, out, kept, wide, sems):
    pairs = ((gate_b, wide.at[0]), (up_b, wide.at[1]), (down_b, kept))
    copies = [pltpu.make_async_copy(*pairs[i], sems.at[i]) for i in range(len(pairs))]
    for copy in copies:
        copy.start()
    inner = wide.shape[2]

    def acts(gated, lifted):
        return (gated / (1.0 + jnp.exp(-gated)) * lifted).astype(jnp.bfloat16)

    out[:, inner:] = acts(dot(x[...], gate_a[...]), dot(x[...], up_a[...]))
    copies[0].wait()
    gated = dot(x[...], wide[0])
    copies[1].wait()
    out[:, :inner] = acts(gated, dot(x[...], wide[1]))
    copies[2].wait()


def products(acts, down_a, down_b, out, flat):
    inner = down_a.shape[0]

    def piece(span):
        return dot(acts[:, :inner], down_b[:, span]) + dot(acts[:, inner:], down_a[:, span])

    row_major(piece, down_a.shape[1], flat, out)


def share(partner, place, gathered, high, low, down, out):
    core = place[0]
    half = 1 - core if partner else core
    columns = gathered.shape[0]
    groups = high.shape[1] // columns
    here = pl.ds(pl.multiple_of(half * groups, groups), groups)
    values = jnp.concatenate([gathered[c, here] for c in range(columns)], axis=0)
    act = jnp.concatenate([gathered[c, 2 * groups :] for c in range(columns)], axis=0)
    mixed = dot(jnp.concatenate([high[...], low[...]], axis=0), values)
    mixed = mixed[: high.shape[0]] + mixed[high.shape[0] :]
    out[...] = mixed + dot(act, down[...], ((0,), (0,)))


def in_vmem(body, shape, *args, dtype=jnp.bfloat16, second=None, smem=0, anywhere=(), scratch=(), onward=False, room=12):
    specs = []
    args = list(args)
    for i in range(len(args)):
        space = pltpu.SMEM if i < smem else pltpu.HBM if i in anywhere else pltpu.VMEM
        specs.append(pl.BlockSpec(memory_space=space))
        if i >= smem and not INTERPRET:
            args[i] = pltpu.with_memory_space_constraint(args[i], space)
    out = jax.ShapeDtypeStruct(shape, dtype)
    shapes = pltpu.VMEM(shape, dtype) if onward and not INTERPRET else out
    out_specs = pl.BlockSpec(memory_space=pltpu.VMEM)
    if second is not None:
        more = jax.ShapeDtypeStruct(second, dtype) if INTERPRET else pltpu.VMEM(second, dtype)
        shapes, out_specs = (shapes, more), (out_specs, out_specs)
    return pl.pallas_call(
        body,
        out_shape=shapes,
        in_specs=specs,
        out_specs=out_specs,
        scratch_shapes=list(scratch),
        interpret=INTERPRET,
        compiler_params=pltpu.CompilerParams(vmem_limit_bytes=room << 20),
    )(*args)


def late_work(tokens, norm_gain, expert_ids, route_weights, shared_gate, shared_up, groups):
    columns = lax.axis_size("x")
    rows, top_count = expert_ids.shape
    as_float = tokens.astype(jnp.float32)
    inverse_rms = lax.rsqrt(jnp.mean(as_float * as_float, axis=-1, keepdims=True) + NORM_EPSILON)
    normed = (as_float * inverse_rms * norm_gain).astype(jnp.bfloat16)

    shared_act = (
        jax.nn.silu(dot(shared_gate, normed, ((0,), (1,)))) * dot(shared_up, normed, ((0,), (1,)))
    ).astype(jnp.bfloat16)

    token_iota = jnp.arange(rows, dtype=jnp.int32)
    strict_lower = (token_iota[:, None] > token_iota[None, :]).astype(jnp.bfloat16)

    slot_iota = jnp.arange(columns * groups, dtype=jnp.int32)
    slot_expert = (slot_iota % groups) * columns + slot_iota // groups
    slot_number = lax.axis_index("core").astype(jnp.float32)
    weight = jnp.zeros((rows, columns * groups), jnp.float32)
    taken = jnp.zeros((rows, columns * groups), jnp.bool_)
    for k in range(top_count):
        hit = expert_ids[:, k : k + 1] == slot_expert[None, :]
        taken = taken | hit
        weight = jnp.where(hit, route_weights[:, k : k + 1], weight)
    ahead = dot(strict_lower, taken.astype(jnp.bfloat16))
    weight = jnp.where(ahead == slot_number, weight, 0.0)
    high = lax.reduce_precision(weight, 8, 7)
    parts = (high.astype(jnp.bfloat16), (weight - high).astype(jnp.bfloat16))
    return shared_act, parts


def local(
    tokens,
    norm_gain,
    expert_ids,
    route_weights,
    expert_gate,
    expert_up,
    expert_down,
    shared_gate,
    shared_up,
    shared_down,
):
    groups = lax.axis_size(EP)
    columns = lax.axis_size("x")
    cores = lax.axis_size("core")
    core = lax.axis_index("core")
    rows, width = tokens.shape
    top_count = expert_ids.shape[1]
    tp_count = columns * cores
    block = width // tp_count

    flat = (groups * tp_count, block)
    buffer = in_vmem(
        functools.partial(pick_rows, columns, cores),
        flat,
        lax.axis_index(TP)[None],
        expert_ids.T,
        tokens,
        norm_gain[None],
        smem=1,
        anywhere=range(1, 4),
        onward=True,
        scratch=(
            pltpu.VMEM((top_count, rows), jnp.int32),
            pltpu.VMEM((rows, width), jnp.bfloat16),
            pltpu.VMEM((1, width), jnp.float32),
            pltpu.VMEM((groups, width), jnp.float32),
            pltpu.VMEM(flat, jnp.float32),
            pltpu.SemaphoreType.DMA((3,)),
        ),
    )
    received = lax.all_to_all(
        buffer.reshape(groups, tp_count, block), EP, split_axis=0, concat_axis=0, tiled=True
    )

    swap = [(0, 1), (1, 0)]
    halves = []
    for half in (expert_gate, expert_up, expert_down):
        halves.append((half[0], lax.ppermute(half[0], "core", swap)))
    gates, ups, downs = halves

    inner = expert_gate.shape[2]
    acts, down_kept = in_vmem(
        hidden_units,
        (groups, 2 * inner),
        received.reshape(groups, width),
        gates[1],
        ups[1],
        gates[0],
        ups[0],
        downs[0],
        second=(inner, width),
        anywhere=range(3, 6),
        onward=True,
        scratch=(pltpu.VMEM((2, width, inner), jnp.bfloat16), pltpu.SemaphoreType.DMA((3,))),
    )
    expert_out = in_vmem(
        products, flat, acts, downs[1], down_kept, onward=True, scratch=(pltpu.VMEM(flat, jnp.float32),)
    )
    returned = lax.all_to_all(expert_out.reshape(groups, tp_count, block), EP, split_axis=0, concat_axis=0, tiled=True)
    shared_act, parts = late_work(
        tokens, norm_gain, expert_ids, route_weights, shared_gate, shared_up, groups
    )
    by_core = shared_down.reshape(columns, cores, -1, block)
    down_own, down_lent = (
        lax.dynamic_index_in_dim(by_core, half, 1, keepdims=False).reshape(-1, block)
        for half in (core, 1 - core)
    )
    down_borrowed = lax.ppermute(down_lent, "core", swap)

    payload = jnp.concatenate(
        [
            jnp.swapaxes(returned, 0, 1).reshape(columns, cores * groups, block),
            jnp.broadcast_to(shared_act[None], (columns,) + shared_act.shape),
        ],
        axis=1,
    )
    payload, down_borrowed, *parts = lax.optimization_barrier((payload, down_borrowed, *parts))
    gathered = lax.all_to_all(payload, "x", split_axis=0, concat_axis=0, tiled=True)
    place = core[None]
    halves = []
    for partner, down in ((True, down_borrowed), (False, down_own)):
        halves.append(
            in_vmem(
                functools.partial(share, partner),
                (rows, block),
                place,
                gathered,
                *parts,
                down,
                dtype=jnp.float32,
                smem=1,
                onward=True,
            )
        )
    from_partner = lax.ppermute(halves[0], "core", swap)
    return (halves[1] + from_partner).astype(jnp.bfloat16)


def solution(mesh):
    ep = mesh.shape["ep"]
    tp = mesh.shape["tp"]
    finer = Mesh(mesh.devices.reshape(8, ep // 8, tp // 2, 2), ALL)
    in_specs = (
        P(EP, None),
        P(),
        P(EP, None),
        P(EP, None),
        P(ALL, None, None),
        P(ALL, None, None),
        P(ALL, None, None),
        P(None, TP),
        P(None, TP),
        P(None, TP),
    )
    out_specs = P(EP, TP)

    return jax.shard_map(local, mesh=finer, in_specs=in_specs, out_specs=out_specs, check_vma=False)
```

```python
import functools

import jax
import jax.numpy as jnp
from jax import lax
from jax.experimental import pallas as pl
from jax.experimental.pallas import tpu as pltpu
from jax.sharding import Mesh
from jax.sharding import PartitionSpec as P


TP = ("x", "core")
EP = ("z", "y")
ALL = ("z", "y", "x", "core")

NORM_EPSILON = 1e-06
INTERPRET = False


def dot(a, b, dims=((1,), (0,))):
    return lax.dot_general(a, b, (dims, ((), ())), preferred_element_type=jnp.float32)


def row_major(piece, width, scratch, packed, out, sems):
    block = out.shape[1]
    count = width // block
    rows = out.shape[0] // count
    for first in range(0, count, 2):
        value = piece(slice(first * block, (first + 2) * block))
        for b in range(2):
            here = value[:, b * block : (b + 1) * block]
            scratch[pl.ds(first + b, rows, stride=count), :] = here
    parts = sems.shape[0]
    size = out.shape[0] // parts
    copies = []
    for i in range(parts):
        span = pl.ds(i * size, size)
        packed[span, :] = scratch[span, :].astype(jnp.bfloat16)
        copies.append(pltpu.make_async_copy(packed.at[span], out.at[span], sems.at[i]))
        copies[-1].start()
    for copy in copies:
        copy.wait()


def pick_rows(columns, cores, place, far_ids, far_tokens, far_gain, out, ids, tokens, gain, picked, wide, packed, sems, out_sems):
    pairs = ((far_ids, ids), (far_tokens, tokens), (far_gain, gain))
    copies = [pltpu.make_async_copy(*pairs[i], sems.at[i]) for i in range(len(pairs))]
    for copy in copies:
        copy.start()
    column, core = place[0] // cores, place[0] % cores
    top_count, rows = ids.shape
    width = tokens.shape[1]
    groups = out.shape[0] * out.shape[1] // width
    expert = lax.broadcasted_iota(jnp.int32, (groups, rows), 0) * columns + column
    copies[0].wait()
    own = ids[0:1, :] == expert
    for k in range(1, top_count):
        own = own | (ids[k : k + 1, :] == expert)
    own = jnp.where(own, 1.0, 0.0)
    sooner = lax.broadcasted_iota(jnp.int32, (rows, rows), 0) < lax.broadcasted_iota(
        jnp.int32, (rows, rows), 1
    )
    before = dot(own.astype(jnp.bfloat16), jnp.where(sooner, 1.0, 0.0).astype(jnp.bfloat16))
    chosen = jnp.where(before == core.astype(jnp.float32), own, 0.0).astype(jnp.bfloat16)
    copies[1].wait()
    step = 2 * out.shape[1]
    spans = [slice(first, first + step) for first in range(0, width, step)]
    squares = jnp.zeros((groups, step), jnp.float32)
    for span in spans:
        row = dot(chosen, tokens[:, span])
        picked[:, span] = row
        squares = squares + row * row
    mean = jnp.sum(squares, axis=1, keepdims=True) * (1.0 / width)
    scale = lax.rsqrt(mean + NORM_EPSILON)
    copies[2].wait()
    row_major(lambda span: picked[:, span] * scale * gain[:, span], width, wide, packed, out, out_sems)


def hidden_units(x, gate_a, up_a, gate_b, up_b, down_b, out, kept, wide, sems):
    pairs = ((gate_b, wide.at[0]), (up_b, wide.at[1]), (down_b, kept))
    copies = [pltpu.make_async_copy(*pairs[i], sems.at[i]) for i in range(len(pairs))]
    for copy in copies:
        copy.start()
    inner = wide.shape[2]

    def acts(gated, lifted):
        return (gated / (1.0 + jnp.exp(-gated)) * lifted).astype(jnp.bfloat16)

    out[:, inner:] = acts(dot(x[...], gate_a[...]), dot(x[...], up_a[...]))
    copies[0].wait()
    gated = dot(x[...], wide[0])
    copies[1].wait()
    out[:, :inner] = acts(gated, dot(x[...], wide[1]))
    copies[2].wait()


def products(acts, down_a, down_b, out, flat, packed, out_sems):
    inner = down_a.shape[0]

    def piece(span):
        return dot(acts[:, :inner], down_b[:, span]) + dot(acts[:, inner:], down_a[:, span])

    row_major(piece, down_a.shape[1], flat, packed, out, out_sems)


def share(partner, place, gathered, high, low, down, out):
    core = place[0]
    half = 1 - core if partner else core
    columns = gathered.shape[0]
    groups = high.shape[1] // columns
    here = pl.ds(pl.multiple_of(half * groups, groups), groups)
    values = jnp.concatenate([gathered[c, here] for c in range(columns)], axis=0)
    act = jnp.concatenate([gathered[c, 2 * groups :] for c in range(columns)], axis=0)
    mixed = dot(jnp.concatenate([high[...], low[...]], axis=0), values)
    mixed = mixed[: high.shape[0]] + mixed[high.shape[0] :]
    out[...] = mixed + dot(act, down[...], ((0,), (0,)))


def in_vmem(body, shape, *args, dtype=jnp.bfloat16, second=None, smem=0, anywhere=(), scratch=(), onward=False, far=False, room=12):
    specs = []
    args = list(args)
    for i in range(len(args)):
        space = pltpu.SMEM if i < smem else pltpu.HBM if i in anywhere else pltpu.VMEM
        specs.append(pl.BlockSpec(memory_space=space))
        if i >= smem and not INTERPRET:
            args[i] = pltpu.with_memory_space_constraint(args[i], space)
    out = jax.ShapeDtypeStruct(shape, dtype)
    shapes = pltpu.VMEM(shape, dtype) if onward and not INTERPRET else out
    out_specs = pl.BlockSpec(memory_space=pltpu.HBM if far else pltpu.VMEM)
    if second is not None:
        more = jax.ShapeDtypeStruct(second, dtype) if INTERPRET else pltpu.VMEM(second, dtype)
        shapes, out_specs = (shapes, more), (out_specs, out_specs)
    return pl.pallas_call(
        body,
        out_shape=shapes,
        in_specs=specs,
        out_specs=out_specs,
        scratch_shapes=list(scratch),
        interpret=INTERPRET,
        compiler_params=pltpu.CompilerParams(vmem_limit_bytes=room << 20),
    )(*args)


def late_work(tokens, norm_gain, expert_ids, route_weights, shared_gate, shared_up, groups):
    columns = lax.axis_size("x")
    rows, top_count = expert_ids.shape
    as_float = tokens.astype(jnp.float32)
    inverse_rms = lax.rsqrt(jnp.mean(as_float * as_float, axis=-1, keepdims=True) + NORM_EPSILON)
    normed = (as_float * inverse_rms * norm_gain).astype(jnp.bfloat16)

    shared_act = (
        jax.nn.silu(dot(shared_gate, normed, ((0,), (1,)))) * dot(shared_up, normed, ((0,), (1,)))
    ).astype(jnp.bfloat16)

    token_iota = jnp.arange(rows, dtype=jnp.int32)
    strict_lower = (token_iota[:, None] > token_iota[None, :]).astype(jnp.bfloat16)

    slot_iota = jnp.arange(columns * groups, dtype=jnp.int32)
    slot_expert = (slot_iota % groups) * columns + slot_iota // groups
    slot_number = lax.axis_index("core").astype(jnp.float32)
    weight = jnp.zeros((rows, columns * groups), jnp.float32)
    taken = jnp.zeros((rows, columns * groups), jnp.bool_)
    for k in range(top_count):
        hit = expert_ids[:, k : k + 1] == slot_expert[None, :]
        taken = taken | hit
        weight = jnp.where(hit, route_weights[:, k : k + 1], weight)
    ahead = dot(strict_lower, taken.astype(jnp.bfloat16))
    weight = jnp.where(ahead == slot_number, weight, 0.0)
    high = lax.reduce_precision(weight, 8, 7)
    parts = (high.astype(jnp.bfloat16), (weight - high).astype(jnp.bfloat16))
    return shared_act, parts


def local(
    tokens,
    norm_gain,
    expert_ids,
    route_weights,
    expert_gate,
    expert_up,
    expert_down,
    shared_gate,
    shared_up,
    shared_down,
):
    groups = lax.axis_size(EP)
    columns = lax.axis_size("x")
    cores = lax.axis_size("core")
    core = lax.axis_index("core")
    rows, width = tokens.shape
    top_count = expert_ids.shape[1]
    tp_count = columns * cores
    block = width // tp_count

    flat = (groups * tp_count, block)
    buffer = in_vmem(
        functools.partial(pick_rows, columns, cores),
        flat,
        lax.axis_index(TP)[None],
        expert_ids.T,
        tokens,
        norm_gain[None],
        smem=1,
        anywhere=range(1, 4),
        far=True,
        scratch=(
            pltpu.VMEM((top_count, rows), jnp.int32),
            pltpu.VMEM((rows, width), jnp.bfloat16),
            pltpu.VMEM((1, width), jnp.float32),
            pltpu.VMEM((groups, width), jnp.float32),
            pltpu.VMEM(flat, jnp.float32),
            pltpu.VMEM(flat, jnp.bfloat16),
            pltpu.SemaphoreType.DMA((3,)),
            pltpu.SemaphoreType.DMA((4,)),
        ),
    )
    received = lax.all_to_all(
        buffer.reshape(groups, tp_count, block), EP, split_axis=0, concat_axis=0, tiled=True
    )

    swap = [(0, 1), (1, 0)]
    halves = []
    for half in (expert_gate, expert_up, expert_down):
        halves.append((half[0], lax.ppermute(half[0], "core", swap)))
    gates, ups, downs = halves

    inner = expert_gate.shape[2]
    acts, down_kept = in_vmem(
        hidden_units,
        (groups, 2 * inner),
        received.reshape(groups, width),
        gates[1],
        ups[1],
        gates[0],
        ups[0],
        downs[0],
        second=(inner, width),
        anywhere=range(3, 6),
        onward=True,
        scratch=(pltpu.VMEM((2, width, inner), jnp.bfloat16), pltpu.SemaphoreType.DMA((3,))),
    )
    expert_out = in_vmem(
        products,
        flat,
        acts,
        downs[1],
        down_kept,
        far=True,
        scratch=(
            pltpu.VMEM(flat, jnp.float32),
            pltpu.VMEM(flat, jnp.bfloat16),
            pltpu.SemaphoreType.DMA((4,)),
        ),
    )
    returned = lax.all_to_all(expert_out.reshape(groups, tp_count, block), EP, split_axis=0, concat_axis=0, tiled=True)
    shared_act, parts = late_work(
        tokens, norm_gain, expert_ids, route_weights, shared_gate, shared_up, groups
    )
    by_core = shared_down.reshape(columns, cores, -1, block)
    down_own, down_lent = (
        lax.dynamic_index_in_dim(by_core, half, 1, keepdims=False).reshape(-1, block)
        for half in (core, 1 - core)
    )
    down_borrowed = lax.ppermute(down_lent, "core", swap)

    payload = jnp.concatenate(
        [
            jnp.swapaxes(returned, 0, 1).reshape(columns, cores * groups, block),
            jnp.broadcast_to(shared_act[None], (columns,) + shared_act.shape),
        ],
        axis=1,
    )
    payload, down_borrowed, *parts = lax.optimization_barrier((payload, down_borrowed, *parts))
    gathered = lax.all_to_all(payload, "x", split_axis=0, concat_axis=0, tiled=True)
    place = core[None]
    halves = []
    for partner, down in ((True, down_borrowed), (False, down_own)):
        halves.append(
            in_vmem(
                functools.partial(share, partner),
                (rows, block),
                place,
                gathered,
                *parts,
                down,
                dtype=jnp.float32,
                smem=1,
                onward=True,
            )
        )
    from_partner = lax.ppermute(halves[0], "core", swap)
    return (halves[1] + from_partner).astype(jnp.bfloat16)


def solution(mesh):
    ep = mesh.shape["ep"]
    tp = mesh.shape["tp"]
    finer = Mesh(mesh.devices.reshape(8, ep // 8, tp // 2, 2), ALL)
    in_specs = (
        P(EP, None),
        P(),
        P(EP, None),
        P(EP, None),
        P(ALL, None, None),
        P(ALL, None, None),
        P(ALL, None, None),
        P(None, TP),
        P(None, TP),
        P(None, TP),
    )
    out_specs = P(EP, TP)

    return jax.shard_map(local, mesh=finer, in_specs=in_specs, out_specs=out_specs, check_vma=False)
```
